256 devices in a mesh: grp: 2 (over z), kv: 16 (over y, core), tp: 8 (over x).
Axes of the slice: x: 8, y: 8, z: 2, core: 2. Of those that a mesh axis runs over, the one named last changes fastest.
The devices are a block of a 8x8x16 slice.
Arguments:
- tokens: bfloat16 [512, 4096], P('grp', ('kv', 'tp')), parts along dimension 0, may hold values from -20 to 20, as said below
- norm_gain: bfloat16 [4096], P('kv'), may hold values from 0.099609375 to 1.8984375
- w_query: bfloat16 [4096, 2048], P('kv', 'tp'), may hold values from -0.09375 to 0.09375
- w_key: bfloat16 [4096, 2048], P('kv', 'tp'), may hold values from -0.09375 to 0.09375
- w_value: bfloat16 [4096, 4096], P('kv', 'tp'), may hold values from -0.09375 to 0.09375
- w_outgate: bfloat16 [4096, 4096], P('kv', 'tp'), may hold values from -0.09375 to 0.09375
- w_input_gate: bfloat16 [4096, 32], P('kv'), may hold values from -0.09375 to 0.09375
- w_forget_gate: bfloat16 [4096, 32], P('kv'), may hold values from -0.09375 to 0.09375
- memory: float32 [512, 32, 64, 128], P(('grp', 'kv'), 'tp'), parts along dimension 0, may hold values from -4 to 4
- normalizer: float32 [512, 32, 64], P(('grp', 'kv'), 'tp'), parts along dimension 0, may hold values from -4 to 4
- stabilizer: float32 [512, 32], P(('grp', 'kv'), 'tp'), parts along dimension 0, may hold values from -4 to 4
- w_mix_out: bfloat16 [4096, 4096], P('tp', 'kv'), may hold values from -0.09375 to 0.09375
- ffn_gain: bfloat16 [4096], P('kv'), may hold values from 0.099609375 to 1.8984375
- w_gate: bfloat16 [4096, 11264], P('kv', 'tp'), may hold values from -0.09375 to 0.09375
- w_up: bfloat16 [4096, 11264], P('kv', 'tp'), may hold values from -0.09375 to 0.09375
- w_down: bfloat16 [11264, 4096], P('tp', 'kv'), may hold values from -0.3125 to 0.3125
Outputs:
- layer_out: bfloat16 [512, 4096], P('grp', ('kv', 'tp')), parts along dimension 0
- new_memory: float32 [512, 32, 64, 128], P(('grp', 'kv'), 'tp'), parts along dimension 0
- new_normalizer: float32 [512, 32, 64], P(('grp', 'kv'), 'tp'), parts along dimension 0
- new_stabilizer: float32 [512, 32], P(('grp', 'kv'), 'tp'), parts along dimension 0
The draws below stay inside these ranges and needn't reach their ends.
There are 2 independent parts, one for each index of `grp`. The reference program is written for one: setup_inputs(seed, part) draws one part's arguments, and reference() takes and returns one part's arrays. A program takes and returns all parts, laid end to end along the dimension named above; an argument that names none is the same for every part. Nothing has to cross between parts.
Inputs may be any that keep to these rules, and one draw needn't show every extreme that they name: tokens' feature scales differ by column and by sequence.
All inputs are finite; a program needn't handle non-finite values.
Results may differ from the reference program's by a relative error of at most 0.029.
Values may be sent and summed in bfloat16 or wider, within the bound.
No kernel may reach another device: no remote copies, remote signals or barrier semaphores. Data moves between devices by JAX's collectives and lax.ppermute only.
A program may use at most 64 MiB of HBM per device.

```python
import jax
import jax.numpy as jnp
from jax import lax

D = 4096
NH = 32
DQK = 64
DV = 128
FF = 11264
SEQS = 256
N_TP = 8


def draw_tokens(key, part):
    base_key, col_key, row_key = jax.random.split(jax.random.fold_in(key, 11), 3)
    columns = jnp.arange(D, dtype=jnp.float32) / (D - 1)
    col_scale = 0.1 * 10.0 ** columns * jax.random.uniform(col_key, (D,), jnp.float32, 0.7, 1.3)
    row_factor = 10.0 ** (jax.random.uniform(row_key, (SEQS, 1), jnp.float32) - 0.5)
    base = jnp.clip(jax.random.normal(base_key, (SEQS, D), jnp.float32), -4.0, 4.0)
    return (base * col_scale[None, :] * row_factor).astype(jnp.bfloat16)


def draw_stabilizer(key, part):
    base_key = jax.random.fold_in(jax.random.fold_in(key, 23), 0)
    base = jax.random.uniform(base_key, (SEQS, NH), jnp.float32, -4.0, 4.0)
    return base


def raised(array, key, source, target, parts, factor):
    def block_of(position):
        return (jnp.arange(array.shape[position]) // (array.shape[position] // parts)).reshape((-1,) + (1,) * (array.ndim - 1 - position))

    near = jax.random.permutation(key, parts)[block_of(target)]
    second = (block_of(target) + parts // 2) % parts
    return jnp.where((block_of(source) == near) | (block_of(source) == second), factor * array, array)


def block_scale(own_key, extent, shards, least, top_value):
    def one(position, shards_of):
        steps = jax.random.uniform(jax.random.fold_in(jax.random.fold_in(own_key, 6), position), (shards_of,), jnp.float32, least / len(shards), top_value / len(shards))
        return jnp.repeat(jnp.exp(steps), extent[position] // shards_of).reshape((-1,) + (1,) * (len(extent) - position - 1))

    gain = one(*shards[0])
    for cut in shards[1:]:
        gain = gain * one(*cut)
    return gain


def gaussian(rng, shape, spread, most, cuts=(), kind=jnp.bfloat16):
    result = spread * jax.random.normal(rng, shape, jnp.float32)
    if cuts:
        result = result * block_scale(rng, shape, cuts, -0.22, 0.18)
    return jnp.clip(result, -most, most).astype(kind)


def noise_with(key, shape, deviation, most, cuts, heavy, kind=jnp.bfloat16):
    array = deviation * jax.random.normal(key, shape, jnp.float32)
    if cuts:
        array = array * block_scale(key, shape, cuts, -0.22, 0.18)
    return jnp.clip(raised(array, jax.random.fold_in(key, 3), *heavy), -most, most).astype(kind)


def setup_inputs(seed: int = 0, part: int = 0) -> dict:
    key_of = jax.random.split(jax.random.key(seed), 17)
    part_keys = jax.random.split(jax.random.fold_in(key_of[16], part), 17)
    return {
        "tokens": draw_tokens(jax.random.fold_in(jax.random.fold_in(key_of[16], part), 71), part),
        "norm_gain": jnp.clip(1.0 + 0.18 * jax.random.normal(key_of[1], (D,), jnp.float32), 0.099609375, 1.8984375).astype(jnp.bfloat16),
        "w_query": gaussian(key_of[2], (D, NH * DQK), D ** -0.5, 0.09375, ((0, 16), (1, 8))),
        "w_key": gaussian(key_of[3], (D, NH * DQK), D ** -0.5, 0.09375, ((0, 16), (1, 8))),
        "w_value": gaussian(key_of[4], (D, NH * DV), D ** -0.5, 0.09375, ((0, 16), (1, 8))),
        "w_outgate": gaussian(key_of[5], (D, NH * DV), D ** -0.5, 0.09375, ((0, 16), (1, 8))),
        "w_input_gate": gaussian(key_of[6], (D, NH), D ** -0.5, 0.09375, ((0, 16),)),
        "w_forget_gate": gaussian(key_of[7], (D, NH), D ** -0.5, 0.09375, ((0, 16),)),
        "memory": gaussian(part_keys[8], (SEQS, NH, DQK, DV), 0.5, 4.0, ((0, 16), (1, 8)), jnp.float32),
        "normalizer": gaussian(part_keys[9], (SEQS, NH, DQK), 0.5, 4.0, ((0, 16), (1, 8)), jnp.float32),
        "stabilizer": draw_stabilizer(jax.random.fold_in(jax.random.fold_in(key_of[16], part), 71), part),
        "w_mix_out": gaussian(key_of[11], (NH * DV, D), (NH * DV) ** -0.5, 0.09375, ((0, 8), (1, 16))),
        "ffn_gain": jnp.clip(1.0 + 0.18 * jax.random.normal(key_of[12], (D,), jnp.float32), 0.099609375, 1.8984375).astype(jnp.bfloat16),
        "w_gate": gaussian(key_of[13], (D, FF), D ** -0.5, 0.09375, ((0, 16), (1, 8))),
        "w_up": gaussian(key_of[14], (D, FF), D ** -0.5, 0.09375, ((0, 16), (1, 8))),
        "w_down": noise_with(key_of[15], (FF, D), (FF // 16) ** -0.5, 0.3125, ((0, 8), (1, 16)), (0, 1, 16, 2.0)),
    }


def row_scale(values):
    wide = values.astype(jnp.float32)
    return lax.rsqrt(lax.optimization_barrier(jnp.mean(wide * wide, axis=-1, keepdims=True)) + 1e-06)

def block_sum(left, right, blocks):
    rows = left.shape[0]
    inner = left.shape[1] // blocks
    left_b = left.reshape(rows, blocks, inner).transpose(1, 0, 2)
    right_b = right.reshape(blocks, inner, right.shape[1])

    def one_block(pair):
        partial_value = jnp.dot(pair[0], pair[1], preferred_element_type=jnp.float32)
        return partial_value.astype(jnp.bfloat16).astype(jnp.float32)
    return lax.optimization_barrier(jnp.sum(lax.map(one_block, (left_b, right_b)), axis=0))

def reference(tokens, norm_gain, w_query, w_key, w_value, w_outgate, w_input_gate, w_forget_gate, memory, normalizer, stabilizer, w_mix_out, ffn_gain, w_gate, w_up, w_down):
    seqs = tokens.shape[0]
    scale1 = row_scale(tokens)
    normed1 = (tokens.astype(jnp.float32) * norm_gain.astype(jnp.float32)).astype(jnp.bfloat16)

    def project(weight):
        return scale1 * jnp.dot(normed1, weight, preferred_element_type=jnp.float32)
    query = project(w_query).reshape(seqs, NH, DQK) * DQK ** (-0.5)
    key = project(w_key).reshape(seqs, NH, DQK)
    value = project(w_value).reshape(seqs, NH, DV)
    outgate = project(w_outgate)
    igate = project(w_input_gate)
    lforget = jax.nn.log_sigmoid(project(w_forget_gate))
    new_stabilizer = jnp.maximum(lforget + stabilizer, igate)
    decay = jnp.exp(lforget + stabilizer - new_stabilizer)
    inflow = jnp.exp(igate - new_stabilizer)
    new_memory = decay[:, :, None, None] * memory + inflow[:, :, None, None] * key[:, :, :, None] * value[:, :, None, :]
    new_normalizer = decay[:, :, None] * normalizer + inflow[:, :, None] * key
    numer = jnp.einsum('bhd,bhde->bhe', query, new_memory)
    denom = lax.optimization_barrier(jnp.sum(query * new_normalizer, axis=-1))
    readout = numer / jnp.maximum(jnp.abs(denom), jnp.exp(-new_stabilizer))[:, :, None]
    gated = (jax.nn.sigmoid(outgate) * readout.reshape(seqs, NH * DV)).astype(jnp.bfloat16)
    mixed_in = (tokens.astype(jnp.float32) + block_sum(gated, w_mix_out, N_TP)).astype(jnp.bfloat16)
    scale2 = row_scale(mixed_in)
    normed2 = (mixed_in.astype(jnp.float32) * ffn_gain.astype(jnp.float32)).astype(jnp.bfloat16)
    gate_pre = scale2 * jnp.dot(normed2, w_gate, preferred_element_type=jnp.float32)
    up_pre = scale2 * jnp.dot(normed2, w_up, preferred_element_type=jnp.float32)
    hidden = (jax.nn.silu(gate_pre) * up_pre).astype(jnp.bfloat16)
    layer_out = (mixed_in.astype(jnp.float32) + block_sum(hidden, w_down, N_TP)).astype(jnp.bfloat16)
    return (layer_out, new_memory, new_normalizer, new_stabilizer)
```

```python
import jax
import jax.numpy as jnp
from jax import lax
from jax.sharding import Mesh, PartitionSpec as P

DQK = 64
DV = 128
CORES = 2
LANES = 128
BF = jnp.bfloat16
F32 = jnp.float32


def swapped(array):
    return lax.ppermute(array, "c", [(0, 1), (1, 0)])


def spread(array, axes, count):
    return lax.all_to_all(
        jnp.broadcast_to(array[None], (count, *array.shape)), axes, 0, 0, tiled=True
    )


def exchanged(pieces, axes):
    return lax.all_to_all(pieces, axes, 0, 0, tiled=True)


def tdot(left_t, right):
    return lax.dot_general(left_t, right, (((0,), (0,)), ((), ())), preferred_element_type=F32)


def dot_t(weight, rows):
    return lax.dot_general(weight, rows, (((0,), (1,)), ((), ())), preferred_element_type=F32)


def two_parts(values):
    high = values.astype(BF)
    return high, (values - high.astype(F32)).astype(BF)


def padded(array, width):
    return jnp.pad(array, ((0, 0), (0, width - array.shape[1])))


def shards(
    tokens,
    norm_gain,
    w_query,
    w_key,
    w_value,
    w_outgate,
    w_input_gate,
    w_forget_gate,
    memory,
    normalizer,
    stabilizer,
    w_mix_out,
    ffn_gain,
    w_gate,
    w_up,
    w_down,
):
    ny, nx = lax.axis_size("y"), lax.axis_size("x")
    core, at_x = lax.axis_index("c"), lax.axis_index("x")
    seqs, feats = tokens.shape
    own, heads = memory.shape[:2]
    half = seqs // CORES
    rows = nx * feats
    width = CORES * ny * rows

    w_in = lax.dynamic_slice_in_dim(w_input_gate, at_x * heads, heads, 1)
    w_fg = lax.dynamic_slice_in_dim(w_forget_gate, at_x * heads, heads, 1)
    gates = padded(jnp.concatenate([w_in, w_fg], axis=1), LANES)
    w_first = jnp.concatenate([w_query, w_key, w_value, w_outgate, gates], axis=1)
    w_first_o = swapped(w_first)
    gains = jnp.stack([norm_gain, ffn_gain])
    gains_o = swapped(gains).astype(F32)
    gains = gains.astype(F32)
    w_mix_o = swapped(w_mix_out)
    w_gate_o = swapped(w_gate)
    w_up_o = swapped(w_up)
    w_down_o = swapped(w_down)

    turned = tokens.T.reshape(feats, ny, CORES, own).transpose(2, 0, 1, 3)
    turned = turned.reshape(CORES, 1, feats, half)
    sent = jnp.broadcast_to(turned, (CORES, nx, feats, half)).reshape(-1, feats, half)
    wide = exchanged(sent, ("c", "x")).reshape(CORES, rows, half)
    mine = lax.dynamic_index_in_dim(wide, core, 0, keepdims=False)
    other = lax.dynamic_index_in_dim(wide, 1 - core, 0, keepdims=False)

    def products(pair, at, ours, theirs):
        first = (pair[0].astype(F32) * gains[at][:, None]).astype(BF)
        second = (pair[1].astype(F32) * gains_o[at][:, None]).astype(BF)
        return tdot(first, ours) + tdot(second, theirs)

    def squares(pair):
        return sum(jnp.sum(jnp.square(p.astype(F32)), axis=0) for p in pair)[:, None]

    z = products((mine, other), 0, w_first, w_first_o)
    main = z.shape[1] - LANES
    small = jnp.concatenate([z[:, main : main + 2 * heads], squares((mine, other))], axis=1)
    extra = padded(jnp.concatenate(two_parts(small), axis=1), LANES)
    sent = jnp.concatenate([z[:, :main].astype(BF), extra], axis=1).reshape(ny, own, -1)
    z = jnp.sum(exchanged(sent, "y").astype(F32), axis=0)
    each = 2 * heads + 1
    small = z[:, main : main + each] + z[:, main + each : main + 2 * each]
    scale1 = lax.rsqrt(small[:, 2 * heads :] / width + 1e-06)
    z = scale1 * z[:, :main]
    nq, nv = heads * DQK, heads * DV
    query = z[:, :nq].reshape(own, heads, DQK) * DQK ** (-0.5)
    key = z[:, nq : 2 * nq].reshape(own, heads, DQK)
    value = z[:, 2 * nq : 2 * nq + nv].reshape(own, heads, DV)
    outgate = z[:, 2 * nq + nv :]
    igate = scale1 * small[:, :heads]
    lforget = jax.nn.log_sigmoid(scale1 * small[:, heads : 2 * heads])
    new_stabilizer = jnp.maximum(lforget + stabilizer, igate)
    decay = jnp.exp(lforget + stabilizer - new_stabilizer)
    inflow = jnp.exp(igate - new_stabilizer)
    new_memory = (
        decay[:, :, None, None] * memory
        + inflow[:, :, None, None] * key[:, :, :, None] * value[:, :, None, :]
    )
    new_normalizer = decay[:, :, None] * normalizer + inflow[:, :, None] * key
    numer = jnp.einsum("bhd,bhde->bhe", query, new_memory)
    denom = jnp.sum(query * new_normalizer, axis=-1)
    readout = numer / jnp.maximum(jnp.abs(denom), jnp.exp(-new_stabilizer))[:, :, None]
    gated = (jax.nn.sigmoid(outgate) * readout.reshape(own, nv)).astype(BF)

    gated = spread(gated, "y", ny).reshape(half, nv)
    partial = jnp.stack([dot_t(w_mix_out, gated), dot_t(w_mix_o, gated)]).astype(BF)
    sent = partial.reshape(CORES, nx, feats, half).transpose(1, 0, 2, 3)
    total = jnp.sum(exchanged(sent, "x").astype(F32), axis=0)
    skip = jnp.stack([mine, other]).reshape(CORES, nx, feats, half)
    skip = lax.dynamic_index_in_dim(skip, at_x, 1, keepdims=False)
    mixed_in = (skip.astype(F32) + total).astype(BF)
    mixed_o = swapped(mixed_in[1])

    wide = spread(mixed_in, "x", nx)
    pair = (wide[:, 0].reshape(rows, half), wide[:, 1].reshape(rows, half))
    gate = products(pair, 1, w_gate, w_gate_o)
    up = products(pair, 1, w_up, w_up_o)
    extra = padded(jnp.concatenate(two_parts(squares(pair)), axis=1), LANES)
    sent = jnp.concatenate([gate.astype(BF), up.astype(BF), extra], axis=1).reshape(ny, own, -1)
    z = jnp.sum(exchanged(sent, "y").astype(F32), axis=0)
    ff = gate.shape[1]
    scale2 = lax.rsqrt((z[:, 2 * ff : 2 * ff + 1] + z[:, 2 * ff + 1 : 2 * ff + 2]) / width + 1e-06)
    hidden = (jax.nn.silu(scale2 * z[:, :ff]) * (scale2 * z[:, ff : 2 * ff])).astype(BF)

    hidden = spread(hidden, "y", ny).reshape(half, ff)
    ours, theirs = dot_t(w_down, hidden).astype(BF), dot_t(w_down_o, hidden).astype(BF)
    first = core == 0
    partial = jnp.stack([jnp.where(first, ours, theirs), jnp.where(first, theirs, ours)])
    got = exchanged(partial.reshape(CORES * nx, feats, half), ("c", "x"))
    total = jnp.sum(got.reshape(CORES, nx, feats, half).astype(F32), axis=1)
    kept = mixed_in[0]
    skip = jnp.stack([jnp.where(first, kept, mixed_o), jnp.where(first, mixed_o, kept)])
    out = (skip.astype(F32) + total).astype(BF).reshape(CORES, feats, ny, own)
    layer_out = out.transpose(1, 2, 0, 3).reshape(feats, seqs).T
    return (layer_out, new_memory, new_normalizer, new_stabilizer)


def solution(mesh):
    sizes = mesh.shape
    shape = (sizes["grp"], sizes["kv"] // CORES, CORES, sizes["tp"])
    fine = Mesh(mesh.devices.reshape(shape), ("grp", "y", "c", "x"))
    kv, tp = ("y", "c"), "x"
    every = P("grp", ("y", "c", "x"))
    in_specs = (
        every,
        P(kv),
        P(kv, tp),
        P(kv, tp),
        P(kv, tp),
        P(kv, tp),
        P(kv, None),
        P(kv, None),
        P(("grp", *kv), tp, None, None),
        P(("grp", *kv), tp, None),
        P(("grp", *kv), tp),
        P(tp, kv),
        P(kv),
        P(kv, tp),
        P(kv, tp),
        P(tp, kv),
    )
    out_specs = (
        every,
        P(("grp", *kv), tp, None, None),
        P(("grp", *kv), tp, None),
        P(("grp", *kv), tp),
    )
    return jax.shard_map(shards, mesh=fine, in_specs=in_specs, out_specs=out_specs, check_vma=False)
```
